32 devices in a mesh: grp: 2 (over y), sp: 4 (over z), tp: 4 (over x, core).
Axes of the slice: x: 2, y: 2, z: 4, core: 2. Of those that a mesh axis runs over, the one named last changes fastest.
Arguments:
- target: bfloat16 [1024, 2048], P(('grp', 'sp', 'tp')), parts along dimension 0, may hold values from -5 to 5
- source: bfloat16 [8192, 2048], P(('grp', 'sp', 'tp')), parts along dimension 0, may hold values from -5 to 5
- source_gain: float32 [2048], replicated, may hold values from 0.1 to 1.9
- pre_first: float32 [2048], replicated, may hold values from 0.1 to 1.9
- query_first: bfloat16 [2048, 2048], P(None, 'tp')
- keyval_first: bfloat16 [2048, 1024], P(None, 'tp')
- out_first: bfloat16 [2048, 2048], P('tp'), may hold values from -0.125 to 0.125
- post_first: float32 [2048], replicated, may hold values from 0.1 to 1.9
- ffn_pre: float32 [2048], replicated, may hold values from 0.1 to 1.9
- w_gate: bfloat16 [2048, 2816], P(None, 'tp'), may hold values from -0.125 to 0.125
- w_value: bfloat16 [2048, 2816], P(None, 'tp'), may hold values from -0.125 to 0.125
- conv_gate: float32 [3, 2816], P(None, 'tp'), may hold values from -3.5 to 3.5
- conv_value: float32 [3, 2816], P(None, 'tp'), may hold values from -3.5 to 3.5
- w_down: bfloat16 [2816, 2048], P('tp'), may hold values from -0.109375 to 0.109375
- ffn_post: float32 [2048], replicated, may hold values from 0.1 to 1.9
- pre_second: float32 [2048], replicated, may hold values from 0.1 to 1.9
- query_second: bfloat16 [2048, 2048], P(None, 'tp')
- keyval_second: bfloat16 [2048, 1024], P(None, 'tp')
- out_second: bfloat16 [2048, 2048], P('tp'), may hold values from -0.125 to 0.125
- post_second: float32 [2048], replicated, may hold values from 0.1 to 1.9
Outputs:
- decoded: float32 [1024, 2048], P(('grp', 'sp', 'tp')), parts along dimension 0
The draws below stay inside these ranges and needn't reach their ends.
There are 2 independent parts, one for each index of `grp`. The reference program is written for one: setup_inputs(seed, part) draws one part's arguments, and reference() takes and returns one part's arrays. A program takes and returns all parts, laid end to end along the dimension named above; an argument that names none is the same for every part. Nothing has to cross between parts.
All inputs are finite; a program needn't handle non-finite values.
Results may differ from the reference program's by a relative error of at most 0.04.
Values may be sent and summed in bfloat16 or wider, within the bound.
A program may use at most 128 MiB of HBM per device.

```python
import jax
import jax.numpy as jnp
from jax import lax

D = 2048
HEAD = 128
QH = 16
KVH = 4
FF = 2816
TARGET = 512
SOURCE = 4096
N_TP = 4


def draw_target(key, part):
    rows = jnp.clip(jax.random.normal(jax.random.fold_in(key, 11), (TARGET, D), jnp.float32), -5.0, 5.0)
    return rows.astype(jnp.bfloat16)


def draw_source(key, part):
    rows = jnp.clip(jax.random.normal(jax.random.fold_in(key, 12), (SOURCE, D), jnp.float32), -5.0, 5.0)
    return rows.astype(jnp.bfloat16)


def layer_weights(key, salt):
    drawn_query = jax.random.normal(jax.random.fold_in(key, salt + 1), (D, QH * HEAD), jnp.float32) * D ** (-0.5)
    drawn_keyval = jax.random.normal(jax.random.fold_in(key, salt + 2), (D, KVH, 2, HEAD), jnp.float32) * D ** (-0.5)
    return (drawn_query, drawn_keyval.reshape(D, KVH * 2 * HEAD))


def draw_query_first(key, part):
    return layer_weights(key, 41)[0].astype(jnp.bfloat16)


def draw_keyval_first(key, part):
    return layer_weights(key, 41)[1].astype(jnp.bfloat16)


def draw_query_second(key, part):
    return layer_weights(key, 51)[0].astype(jnp.bfloat16)


def draw_keyval_second(key, part):
    return layer_weights(key, 51)[1].astype(jnp.bfloat16)


def block_levels(stream_key, dims, cuts, smallest, top_value):
    loudness, own = 1.0, jax.random.fold_in(stream_key, 6)
    for dim, shards_of in cuts:
        draws = jnp.exp(jax.random.uniform(jax.random.fold_in(own, dim), (shards_of,), jnp.float32, smallest / len(cuts), top_value / len(cuts)))
        loudness = loudness * jnp.repeat(draws, dims[dim] // shards_of).reshape([-1 if axis == dim else 1 for axis in range(len(dims))])
    return loudness


def bell_draw(own_key, shape, scale, bound, split=(), held_as=jnp.bfloat16):
    result = jax.random.normal(own_key, shape, jnp.float32) * scale
    if len(split) > 0:
        result = block_levels(own_key, shape, split, -0.22, 0.18) * result
    return jnp.clip(result, min=-bound, max=bound).astype(held_as)


def setup_inputs(seed: int = 0, part: int = 0) -> dict:
    key_of = jax.random.split(jax.random.key(seed), 21)
    part_splits = jax.random.split(jax.random.fold_in(key_of[20], part), 21)
    return {
        "target": draw_target(jax.random.fold_in(jax.random.fold_in(key_of[20], part), 71), part),
        "source": draw_source(jax.random.fold_in(jax.random.fold_in(key_of[20], part), 71), part),
        "source_gain": jnp.clip(jax.random.uniform(key_of[2], (D,), jnp.float32, 0.1, 1.9), 0.1, 1.9),
        "pre_first": jnp.clip(jax.random.uniform(key_of[3], (D,), jnp.float32, 0.1, 1.9), 0.1, 1.9),
        "query_first": draw_query_first(jax.random.fold_in(key_of[20], 71), part),
        "keyval_first": draw_keyval_first(jax.random.fold_in(key_of[20], 71), part),
        "out_first": bell_draw(key_of[6], (QH * HEAD, D), (QH * HEAD) ** -0.5, 0.125, ((0, 4),)),
        "post_first": jnp.clip(jax.random.uniform(key_of[7], (D,), jnp.float32, 0.1, 1.9), 0.1, 1.9),
        "ffn_pre": jnp.clip(jax.random.uniform(key_of[8], (D,), jnp.float32, 0.1, 1.9), 0.1, 1.9),
        "w_gate": bell_draw(key_of[9], (D, FF), D ** -0.5, 0.125, ((1, 4),)),
        "w_value": bell_draw(key_of[10], (D, FF), D ** -0.5, 0.125, ((1, 4),)),
        "conv_gate": bell_draw(key_of[11], (3, FF), 3 ** -0.5, 3.5, ((1, 4),), jnp.float32),
        "conv_value": bell_draw(key_of[12], (3, FF), 3 ** -0.5, 3.5, ((1, 4),), jnp.float32),
        "w_down": bell_draw(key_of[13], (FF, D), FF ** -0.5, 0.109375, ((0, 4),)),
        "ffn_post": jnp.clip(jax.random.uniform(key_of[14], (D,), jnp.float32, 0.1, 1.9), 0.1, 1.9),
        "pre_second": jnp.clip(jax.random.uniform(key_of[15], (D,), jnp.float32, 0.1, 1.9), 0.1, 1.9),
        "query_second": draw_query_second(jax.random.fold_in(key_of[20], 71), part),
        "keyval_second": draw_keyval_second(jax.random.fold_in(key_of[20], 71), part),
        "out_second": bell_draw(key_of[18], (QH * HEAD, D), (QH * HEAD) ** -0.5, 0.125, ((0, 4),)),
        "post_second": jnp.clip(jax.random.uniform(key_of[19], (D,), jnp.float32, 0.1, 1.9), 0.1, 1.9),
    }


def normed(values, gain):
    widened = values.astype(jnp.float32)
    return widened * lax.rsqrt(lax.optimization_barrier(jnp.mean(widened * widened, axis=-1, keepdims=True)) + 1e-06) * gain

def sharded_product(left_side, right_side, shards):
    column_span = left_side.shape[1] // shards

    def accumulate(running, shard_index):
        left_part = lax.dynamic_slice_in_dim(left_side, shard_index * column_span, column_span, 1)
        right_part = lax.dynamic_slice_in_dim(right_side, shard_index * column_span, column_span, 0)
        rounded = jnp.dot(left_part, right_part, preferred_element_type=jnp.float32).astype(jnp.bfloat16)
        rounded = lax.optimization_barrier(rounded)
        return (running + rounded.astype(jnp.float32), None)
    initial = jnp.zeros((left_side.shape[0], right_side.shape[1]), jnp.float32)
    summed, unused = lax.scan(accumulate, initial, jnp.arange(shards, dtype=jnp.int32))
    return summed

def attend(queries, keyvals):
    group_size = QH // KVH
    scale_factor = HEAD ** (-0.5)
    query_heads = jnp.moveaxis(queries.reshape(TARGET, QH, HEAD), 1, 0)

    def one_head(inputs):
        head_queries, head_index = inputs
        columns = lax.dynamic_slice_in_dim(keyvals, head_index // group_size * (2 * HEAD), 2 * HEAD, 1)
        head_keys = columns[:, :HEAD]
        head_values = columns[:, HEAD:]
        scores = lax.dot_general(head_queries, head_keys, (((1,), (1,)), ((), ())), preferred_element_type=jnp.float32) * scale_factor
        row_max = lax.optimization_barrier(jnp.max(scores, axis=1, keepdims=True))
        weights = jnp.exp(scores - row_max)
        weight_sum = lax.optimization_barrier(jnp.sum(weights, axis=1, keepdims=True))
        gathered = jnp.dot(weights.astype(jnp.bfloat16), head_values, preferred_element_type=jnp.float32)
        return (gathered / weight_sum).astype(jnp.bfloat16)
    outputs = lax.map(one_head, (query_heads, jnp.arange(QH, dtype=jnp.int32)))
    return jnp.moveaxis(outputs, 0, 1).reshape(TARGET, QH * HEAD)

def attention_layer(stream, pre_gain, w_query, keyvals, w_out, post_gain):
    hidden = normed(stream, pre_gain).astype(jnp.bfloat16)
    queries = jnp.dot(hidden, w_query, preferred_element_type=jnp.float32).astype(jnp.bfloat16)
    heads = attend(queries, keyvals)
    mixed = sharded_product(heads, w_out, N_TP)
    return stream.astype(jnp.float32) + normed(mixed, post_gain)

def causal_mix(up_rows, conv_taps):
    padded = jnp.pad(up_rows.astype(jnp.float32), ((2, 0), (0, 0)))
    length = up_rows.shape[0]
    return conv_taps[0] * padded[:length] + conv_taps[1] * padded[1:length + 1] + conv_taps[2] * padded[2:]

def reference(target, source, source_gain, pre_first, query_first, keyval_first, out_first, post_first, ffn_pre, w_gate, w_value, conv_gate, conv_value, w_down, ffn_post, pre_second, query_second, keyval_second, out_second, post_second):
    source_normed = normed(source, source_gain).astype(jnp.bfloat16)
    kv_first = jnp.dot(source_normed, keyval_first, preferred_element_type=jnp.float32).astype(jnp.bfloat16)
    kv_second = jnp.dot(source_normed, keyval_second, preferred_element_type=jnp.float32).astype(jnp.bfloat16)
    after_first = attention_layer(target, pre_first, query_first, kv_first, out_first, post_first)
    ffn_input = normed(after_first, ffn_pre).astype(jnp.bfloat16)
    up_gate = jnp.dot(ffn_input, w_gate, preferred_element_type=jnp.float32).astype(jnp.bfloat16)
    up_value = jnp.dot(ffn_input, w_value, preferred_element_type=jnp.float32).astype(jnp.bfloat16)
    gated = (jax.nn.gelu(causal_mix(up_gate, conv_gate), approximate=True) * causal_mix(up_value, conv_value)).astype(jnp.bfloat16)
    ffn_sum = sharded_product(gated, w_down, N_TP)
    after_ffn = after_first + normed(ffn_sum, ffn_post)
    return attention_layer(after_ffn, pre_second, query_second, kv_second, out_second, post_second)
```

```python
import math

import jax
import jax.numpy as jnp
from jax import lax
from jax.experimental import pallas as pl
from jax.experimental.pallas import tpu as pltpu
from jax.sharding import PartitionSpec as P

HEAD = 128
CHUNKS = 4
EXP_SCALE = HEAD ** (-0.5) * math.log2(math.e)
F32, BF16 = jnp.float32, jnp.bfloat16
MESH = pl.DeviceIdType.MESH


def normed(values, gain):
    widened = values.astype(F32)
    return widened * lax.rsqrt(jnp.mean(widened * widened, axis=-1, keepdims=True) + 1e-06) * gain


def times(start, stop, body):
    if stop - start <= 4:
        for index in range(start, stop):
            body(index)
    else:

        @pl.loop(start, stop)
        def _(index):
            body(index)


def dot(left, right):
    return jnp.dot(left, right, preferred_element_type=F32)


def decoder_kernel(
    n_tp,
    n_sp,
    target_h,
    source_h,
    source_gain,
    pre_first,
    query_first_h,
    keyval_first_h,
    out_first_h,
    post_first,
    ffn_pre,
    gate_h,
    value_h,
    conv_gate,
    conv_value,
    down_h,
    ffn_post,
    pre_second,
    query_second_h,
    keyval_second_h,
    out_second_h,
    post_second,
    decoded,
    target_v,
    source_v,
    query_first,
    keyval_first,
    out_first,
    w_gate,
    w_value,
    w_down,
    query_second,
    keyval_second,
    out_second,
    local_sem,
    hidden,
    hidden_sem,
    src,
    src_send,
    src_recv,
    q_slots,
    q_sem,
    k_first,
    v_first,
    k_second,
    v_second,
    kv_send,
    kv_recv,
    run_max,
    run_sum,
    run_out,
    mix_send,
    mix_recv,
    stat_send,
    stat_recv,
    mix_sem,
    part,
    part_recv,
    part_sem,
    halo_send,
    halo_recv,
    halo_sem,
    stream,
):
    me = lax.axis_index("tp")
    z = lax.axis_index("sp")
    sib = me + 1 - 2 * lax.rem(me, 2)
    n_chip = n_tp // 2
    rows = target_v.shape[0]
    width = target_v.shape[1]
    chunk = src.shape[2]
    block_rows = rows * n_tp

    def tp_at(distance):
        return lax.rem(me + distance, n_tp)

    def sp_at(distance):
        return lax.rem(z + distance, n_sp)

    def to_tp(source, dest, send, recv, device):
        return pltpu.make_async_remote_copy(
            src_ref=source, dst_ref=dest, send_sem=send, recv_sem=recv,
            device_id={"tp": device}, device_id_type=MESH,
        )

    def to_sp(source, dest, send, recv, device):
        return pltpu.make_async_remote_copy(
            src_ref=source, dst_ref=dest, send_sem=send, recv_sem=recv,
            device_id={"sp": device}, device_id_type=MESH,
        )

    pairs = [
        (target_h, target_v),
        (source_h, source_v),
        (query_first_h, query_first),
        (keyval_first_h, keyval_first),
        (keyval_second_h, keyval_second),
        (out_first_h, out_first),
        (gate_h, w_gate),
        (value_h, w_value),
        (down_h, w_down),
        (query_second_h, query_second),
        (out_second_h, out_second),
    ]
    loads = [
        pltpu.make_async_copy(a, b, local_sem.at[i]) for i, (a, b) in enumerate(pairs)
    ]
    for load in loads:
        load.start()

    barrier = pltpu.get_barrier_semaphore()
    for distance in range(1, n_tp):
        pl.semaphore_signal(barrier, inc=1, device_id={"tp": tp_at(distance)}, device_id_type=MESH)
    for distance in range(1, n_sp):
        pl.semaphore_signal(barrier, inc=1, device_id={"sp": sp_at(distance)}, device_id_type=MESH)
    pl.semaphore_wait(barrier, n_tp - 1 + n_sp - 1)

    def hidden_copy(phase, slot, device):
        return to_tp(
            hidden.at[phase, slot], hidden.at[phase, slot],
            hidden_sem.at[0, phase, 0], hidden_sem.at[1, phase, slot], device,
        )

    def gather_start(phase, value):
        hidden[phase, me] = value.astype(BF16)
        for d in range(1, n_chip):
            hidden_copy(phase, me, tp_at(2 * d)).start()
        hidden_copy(phase, me, sib).start()

    def gather_finish(phase):
        for d in range(1, n_chip):
            slot = tp_at(2 * d)
            hidden_copy(phase, slot, sib).wait_recv()
            hidden_copy(phase, slot, sib).start()
        hidden_copy(phase, sib, sib).wait_recv()
        for d in range(1, n_chip):
            hidden_copy(phase, lax.rem(sib + 2 * d, n_tp), sib).wait_recv()
        whole = hidden[phase]
        if rows % 16:
            return whole.astype(F32).reshape(block_rows, width).astype(BF16)
        return whole.reshape(block_rows, width)

    def gather_drain(phase):
        for _ in range(2 * n_chip - 1):
            hidden_copy(phase, me, sib).wait_send()

    def part_copy(phase, distance, slot):
        return to_tp(
            part.at[phase, tp_at(distance)], part_recv.at[phase, slot],
            part_sem.at[0, phase, 0], part_sem.at[1, phase, slot], tp_at(distance),
        )

    def scatter_sum(phase, product):
        part[phase] = product.reshape(n_tp, rows, width).astype(BF16)
        order = [d for d in range(1, n_tp) if d != 2] + ([2] if n_tp > 2 else [])
        for d in order:
            part_copy(phase, d, me).start()
        total = part[phase, me].astype(F32)
        for d in range(1, n_tp):
            slot = tp_at(d)
            part_copy(phase, d, slot).wait_recv()
            total = total + part_recv[phase, slot].astype(F32)
        for d in range(1, n_tp):
            part_copy(phase, d, me).wait_send()
        return total

    def head_columns(queries):
        blocks = [
            queries[:, h : h + HEAD].T for h in range(0, queries.shape[1], HEAD)
        ]
        return jnp.concatenate(blocks, axis=1).astype(BF16)

    def head_rows(columns):
        blocks = [
            columns[:, c : c + block_rows].T for c in range(0, columns.shape[1], block_rows)
        ]
        return jnp.concatenate(blocks, axis=1).astype(BF16)

    loads[0].wait()
    gather_start(0, normed(target_v[...], pre_first[...]))

    def src_copy(slot, c, device, kind):
        return to_tp(
            src.at[slot, c], src.at[slot, c], src_send.at[kind], src_recv.at[slot, c], device
        )

    loads[1].wait()
    for c in range(CHUNKS):
        src[me, c] = normed(source_v[pl.ds(c * chunk, chunk)], source_gain[...]).astype(BF16)
        for d in range(1, n_chip):
            src_copy(me, c, tp_at(2 * d), 0).start()
        src_copy(me, c, sib, 0).start()

    loads[2].wait()
    q_slots[z] = head_columns(dot(gather_finish(0), query_first[...]))

    def q_copy(distance, slot):
        return to_sp(
            q_slots.at[z], q_slots.at[z] if slot is None else q_slots.at[slot],
            q_sem.at[0, 0], q_sem.at[1, z if slot is None else slot], sp_at(distance),
        )

    for d in range(1, n_sp):
        q_copy(d, None).start()

    loads[3].wait()
    loads[4].wait()

    def project(lines, block, offset):
        first = dot(lines, keyval_first[...])
        second = dot(lines, keyval_second[...])
        span = pl.ds(offset, lines.shape[0])
        k_first[block, span] = first[:, :HEAD].astype(BF16)
        v_first[block, span] = first[:, HEAD:].astype(BF16)
        k_second[z, block, span] = second[:, :HEAD].astype(BF16)
        v_second[z, block, span] = second[:, HEAD:].astype(BF16)

    def project_pair(block, c, mine, other):
        lines = jnp.concatenate([src[mine, c], src[other, c]], axis=0)
        project(lines, block, c * 2 * chunk)

    def absorb(keys, values, queries, slot, fresh):
        scores = dot(keys, queries)
        newest = jnp.max(scores, axis=0, keepdims=True)
        if not fresh:
            newest = jnp.maximum(newest, run_max[slot])
        weights = jnp.exp2((scores - newest) * EXP_SCALE)
        added = jnp.sum(weights, axis=0, keepdims=True)
        gathered = lax.dot_general(
            values, weights.astype(BF16), (((0,), (0,)), ((), ())), preferred_element_type=F32
        )
        if not fresh:
            rescale = jnp.exp2((run_max[slot] - newest) * EXP_SCALE)
            added = added + run_sum[slot] * rescale
            gathered = gathered + run_out[slot] * rescale
        run_max[slot] = newest
        run_sum[slot] = added
        run_out[slot] = gathered

    def absorb_block(block, fresh):
        @pl.loop(0, n_sp)
        def _(slot):
            absorb(k_first[block], v_first[block], q_slots[slot], slot, fresh)

    def kv_copies(block, slot, distance):
        peer = sp_at(distance)
        return [
            to_sp(
                store.at[z, block], store.at[slot, block],
                kv_send.at[index], kv_recv.at[index, slot, block], peer,
            )
            for index, store in enumerate((k_second, v_second))
        ]

    def kv_start(block):
        def one(d):
            for copy in kv_copies(block, z, d):
                copy.start()

        times(1, n_sp, one)

    for c in range(CHUNKS):
        src_copy(sib, c, sib, 0).wait_recv()
        project_pair(0, c, me, sib)
    for d in range(1, n_sp):
        q_copy(d, sp_at(d)).wait_recv()
    kv_start(0)
    absorb_block(0, True)

    def far_chip(d):
        near = tp_at(2 * d)
        far = lax.rem(sib + 2 * d, n_tp)
        for c in range(CHUNKS):
            src_copy(near, c, sib, 1).wait_recv()
            src_copy(near, c, sib, 1).start()
            src_copy(far, c, sib, 1).wait_recv()
            project_pair(d, c, near, far)
        absorb_block(d, False)

    times(1, n_chip, far_chip)

    def mix_copies(distance, slot):
        peer = sp_at(distance)
        return [
            to_sp(sent.at[peer], got.at[slot], mix_sem.at[index, 0, 0], mix_sem.at[index, 1, slot], peer)
            for index, (sent, got) in enumerate(((mix_send, mix_recv), (stat_send, stat_recv)))
        ]

    @pl.loop(0, n_sp)
    def _(slot):
        total = run_sum[slot]
        mix_send[slot] = (run_out[slot] / total).astype(BF16)
        stat_send[slot] = jnp.concatenate([run_max[slot], total], axis=0)

    for d in range(1, n_sp):
        for copy in mix_copies(d, z):
            copy.start()
    for d in range(1, n_sp):
        for copy in mix_copies(d, sp_at(d)):
            copy.wait_recv()
    for block in range(1, n_chip):
        kv_start(block)
    mix_recv[z] = mix_send[z]
    stat_recv[z] = stat_send[z]
    top = stat_recv[0, 0:1]
    for slot in range(1, n_sp):
        top = jnp.maximum(top, stat_recv[slot, 0:1])
    weight_sum = jnp.zeros_like(top)
    weighted = jnp.zeros(run_out.shape[1:], F32)
    for slot in range(n_sp):
        share = jnp.exp2((stat_recv[slot, 0:1] - top) * EXP_SCALE) * stat_recv[slot, 1:2]
        weight_sum = weight_sum + share
        weighted = weighted + mix_recv[slot].astype(F32) * share
    loads[5].wait()
    mixed = scatter_sum(0, dot(head_rows(weighted / weight_sum), out_first[...]))
    after_first = target_v[...].astype(F32) + normed(mixed, post_first[...])
    stream[...] = after_first

    gather_start(1, normed(after_first, ffn_pre[...]))
    loads[6].wait()
    loads[7].wait()
    ffn_input = gather_finish(1)
    up_gate = dot(ffn_input, w_gate[...]).astype(BF16)
    up_value = dot(ffn_input, w_value[...]).astype(BF16)
    halo_send[0] = up_gate[block_rows - 16 :]
    halo_send[1] = up_value[block_rows - 16 :]
    halo = to_sp(halo_send, halo_recv, halo_sem.at[0], halo_sem.at[1], sp_at(1))

    @pl.when(z < n_sp - 1)
    def _():
        halo.start()

    @pl.when(z > 0)
    def _():
        halo.wait_recv()

    def causal_mix(up_rows, rim, taps):
        here = up_rows.astype(F32)
        rim = jnp.where(z > 0, rim.astype(F32), 0.0)
        row = lax.broadcasted_iota(jnp.int32, here.shape, 0)
        before = jnp.where(row == 0, rim[15:16], pltpu.roll(here, 1, 0))
        earlier = jnp.where(
            row == 0, rim[14:15], jnp.where(row == 1, rim[15:16], pltpu.roll(here, 2, 0))
        )
        return taps[0:1] * earlier + taps[1:2] * before + taps[2:3] * here

    gated = (
        jax.nn.gelu(causal_mix(up_gate, halo_recv[0], conv_gate[...]), approximate=True)
        * causal_mix(up_value, halo_recv[1], conv_value[...])
    ).astype(BF16)
    loads[8].wait()
    ffn_sum = scatter_sum(1, dot(gated, w_down[...]))
    after_ffn = stream[...] + normed(ffn_sum, ffn_post[...])
    stream[...] = after_ffn

    gather_start(2, normed(after_ffn, pre_second[...]))
    loads[9].wait()
    queries = head_columns(dot(gather_finish(2), query_second[...]))
    for d in range(1, n_sp):
        q_copy(d, None).wait_send()
    q_slots[z] = queries

    for block in range(n_chip):
        absorb(k_second[z, block], v_second[z, block], q_slots[z], 0, block == 0)

    def absorb_slot(d):
        slot = sp_at(d)
        for block in range(n_chip):
            for copy in kv_copies(block, slot, d):
                copy.wait_recv()
            absorb(k_second[slot, block], v_second[slot, block], q_slots[z], 0, False)

    times(1, n_sp, absorb_slot)
    loads[10].wait()
    mixed = scatter_sum(2, dot(head_rows(run_out[0] / run_sum[0]), out_second[...]))
    decoded[...] = stream[...] + normed(mixed, post_second[...])

    for phase in range(3):
        gather_drain(phase)
    for c in range(CHUNKS):
        for _ in range(n_chip):
            src_copy(me, c, sib, 0).wait_send()
        for d in range(1, n_chip):
            src_copy(me, c, sib, 1).wait_send()

    def drain(d):
        for block in range(n_chip):
            for copy in kv_copies(block, z, d):
                copy.wait_send()
        for copy in mix_copies(d, z):
            copy.wait_send()

    times(1, n_sp, drain)

    @pl.when(z < n_sp - 1)
    def _():
        halo.wait_send()


def per_device(*arrays):
    (target, source, source_gain, pre_first, query_first, keyval_first, out_first, post_first,
     ffn_pre, w_gate, w_value, conv_gate, conv_value, w_down, ffn_post, pre_second,
     query_second, keyval_second, out_second, post_second) = arrays
    n_tp, n_sp = lax.axis_size("tp"), lax.axis_size("sp")
    sharers = 2 * HEAD // keyval_first.shape[1]
    if sharers > 1:
        groups = [list(range(low, low + sharers)) for low in range(0, n_tp, sharers)]
        keyval_first, keyval_second = (
            lax.all_gather(w, "tp", axis=1, tiled=True, axis_index_groups=groups)
            for w in (keyval_first, keyval_second)
        )
    rows, width = target.shape
    lines = source.shape[0]
    block_rows = rows * n_tp
    columns = query_first.shape[1] // HEAD * block_rows
    hidden_units = w_gate.shape[1]
    n_chip = n_tp // 2
    dma = pltpu.SemaphoreType.DMA
    any_spec = pl.BlockSpec(memory_space=pl.ANY)
    vmem = pl.BlockSpec(memory_space=pltpu.VMEM)

    def row(gain):
        return gain.reshape(1, width)

    scratch = [
        pltpu.VMEM(target.shape, BF16),
        pltpu.VMEM(source.shape, BF16),
        *(pltpu.VMEM(w.shape, BF16) for w in (
            query_first, keyval_first, out_first, w_gate, w_value, w_down,
            query_second, keyval_second, out_second)),
        dma((11,)),
        pltpu.VMEM((3, n_tp, rows, width), BF16),
        dma((2, 3, n_tp)),
        pltpu.VMEM((n_tp, CHUNKS, lines // CHUNKS, width), BF16),
        dma((2,)),
        dma((n_tp, CHUNKS)),
        pltpu.VMEM((n_sp, HEAD, columns), BF16),
        dma((2, n_sp)),
        pltpu.VMEM((n_chip, 2 * lines, HEAD), BF16),
        pltpu.VMEM((n_chip, 2 * lines, HEAD), BF16),
        pltpu.VMEM((n_sp, n_chip, 2 * lines, HEAD), BF16),
        pltpu.VMEM((n_sp, n_chip, 2 * lines, HEAD), BF16),
        dma((2,)),
        dma((2, n_sp, n_chip)),
        pltpu.VMEM((n_sp, 1, columns), F32),
        pltpu.VMEM((n_sp, 1, columns), F32),
        pltpu.VMEM((n_sp, HEAD, columns), F32),
        pltpu.VMEM((n_sp, HEAD, columns), BF16),
        pltpu.VMEM((n_sp, HEAD, columns), BF16),
        pltpu.VMEM((n_sp, 2, columns), F32),
        pltpu.VMEM((n_sp, 2, columns), F32),
        dma((2, 2, n_sp)),
        pltpu.VMEM((3, n_tp, rows, width), BF16),
        pltpu.VMEM((3, n_tp, rows, width), BF16),
        dma((2, 3, n_tp)),
        pltpu.VMEM((2, 16, hidden_units), BF16),
        pltpu.VMEM((2, 16, hidden_units), BF16),
        dma((2,)),
        pltpu.VMEM((rows, width), F32),
    ]

    def kernel(*refs):
        decoder_kernel(n_tp, n_sp, *refs)

    return pl.pallas_call(
        kernel,
        out_shape=jax.ShapeDtypeStruct((rows, width), F32),
        in_specs=[any_spec, any_spec, vmem, vmem, any_spec, any_spec, any_spec, vmem, vmem,
                  any_spec, any_spec, vmem, vmem, any_spec, vmem, vmem, any_spec, any_spec,
                  any_spec, vmem],
        out_specs=vmem,
        scratch_shapes=scratch,
        compiler_params=pltpu.CompilerParams(
            collective_id=0, has_side_effects=True, vmem_limit_bytes=67_000_000
        ),
        name="decoder",
    )(
        target, source, row(source_gain), row(pre_first), query_first, keyval_first, out_first,
        row(post_first), row(ffn_pre), w_gate, w_value, conv_gate, conv_value, w_down,
        row(ffn_post), row(pre_second), query_second, keyval_second, out_second, row(post_second),
    )


def solution(mesh):
    rows = P(("grp", "sp", "tp"), None)
    by_column, by_row = P(None, "tp"), P("tp", None)
    placed = (
        rows, rows, P(), P(), by_column, by_column, by_row, P(), P(), by_column, by_column,
        by_column, by_column, by_row, P(), P(), by_column, by_column, by_row, P(),
    )
    return jax.shard_map(
        per_device, mesh=mesh, in_specs=placed, out_specs=rows, check_vma=False
    )
```

```python
import math

import jax
import jax.numpy as jnp
from jax import lax
from jax.experimental import pallas as pl
from jax.experimental.pallas import tpu as pltpu
from jax.sharding import PartitionSpec as P

HEAD = 128
CHUNKS = 4
PIECES = 2
EXP_SCALE = HEAD ** (-0.5) * math.log2(math.e)
F32, BF16 = jnp.float32, jnp.bfloat16
MESH = pl.DeviceIdType.MESH


def normed(values, gain):
    widened = values.astype(F32)
    return widened * lax.rsqrt(jnp.mean(widened * widened, axis=-1, keepdims=True) + 1e-06) * gain


def times(start, stop, body):
    if stop - start <= 4:
        for index in range(start, stop):
            body(index)
    else:

        @pl.loop(start, stop)
        def _(index):
            body(index)


def dot(left, right):
    return jnp.dot(left, right, preferred_element_type=F32)


def decoder_kernel(
    n_tp,
    n_sp,
    target_h,
    source_h,
    source_gain,
    pre_first,
    query_first_h,
    keyval_first_h,
    out_first_h,
    post_first,
    ffn_pre,
    gate_h,
    value_h,
    conv_gate,
    conv_value,
    down_h,
    ffn_post,
    pre_second,
    query_second_h,
    keyval_second_h,
    out_second_h,
    post_second,
    decoded,
    target_v,
    source_v,
    query_first,
    keyval_first,
    out_first,
    w_gate,
    w_value,
    w_down,
    query_second,
    keyval_second,
    out_second,
    local_sem,
    hidden,
    hidden_send,
    hidden_recv,
    src,
    src_send,
    src_recv,
    q_slots,
    q_sem,
    k_first,
    v_first,
    k_second,
    v_second,
    kv_send,
    kv_recv,
    run_max,
    run_sum,
    run_out,
    mix_send,
    mix_recv,
    stat_send,
    stat_recv,
    mix_sem,
    part,
    pair_recv,
    pair_sum,
    part_recv,
    part_send,
    pair_sem,
    part_sem,
    halo_send,
    halo_recv,
    halo_sem,
    stream,
):
    me = lax.axis_index("tp")
    z = lax.axis_index("sp")
    sib = me + 1 - 2 * lax.rem(me, 2)
    core, chip = lax.rem(me, 2), me // 2
    n_chip = n_tp // 2
    rows = target_v.shape[0]
    width = target_v.shape[1]
    span = width // PIECES
    chunk = src.shape[2]
    block_rows = rows * n_tp

    def tp_at(distance):
        return lax.rem(me + distance, n_tp)

    def sp_at(distance):
        return lax.rem(z + distance, n_sp)

    def to_tp(source, dest, send, recv, device):
        return pltpu.make_async_remote_copy(
            src_ref=source, dst_ref=dest, send_sem=send, recv_sem=recv,
            device_id={"tp": device}, device_id_type=MESH,
        )

    def to_sp(source, dest, send, recv, device):
        return pltpu.make_async_remote_copy(
            src_ref=source, dst_ref=dest, send_sem=send, recv_sem=recv,
            device_id={"sp": device}, device_id_type=MESH,
        )

    pairs = [
        (target_h, target_v),
        (source_h, source_v),
        (query_first_h, query_first),
        (keyval_first_h, keyval_first),
        (keyval_second_h, keyval_second),
        (out_first_h, out_first),
        (gate_h, w_gate),
        (value_h, w_value),
        (down_h, w_down),
        (query_second_h, query_second),
        (out_second_h, out_second),
    ]
    loads = [
        pltpu.make_async_copy(a, b, local_sem.at[i]) for i, (a, b) in enumerate(pairs)
    ]
    for load in loads:
        load.start()

    barrier = pltpu.get_barrier_semaphore()
    for distance in range(1, n_tp):
        pl.semaphore_signal(barrier, inc=1, device_id={"tp": tp_at(distance)}, device_id_type=MESH)
    for distance in range(1, n_sp):
        pl.semaphore_signal(barrier, inc=1, device_id={"sp": sp_at(distance)}, device_id_type=MESH)
    pl.semaphore_wait(barrier, n_tp - 1 + n_sp - 1)

    def hidden_copy(phase, piece, slot, device):
        return to_tp(
            hidden.at[phase, piece, slot], hidden.at[phase, piece, slot],
            hidden_send.at[phase], hidden_recv.at[phase, piece, slot], device,
        )

    def gather_start(phase, value):
        for piece in range(PIECES):
            hidden[phase, piece, me] = value[:, piece * span : (piece + 1) * span].astype(BF16)
            for d in range(1, n_chip):
                hidden_copy(phase, piece, me, tp_at(2 * d)).start()
            hidden_copy(phase, piece, me, sib).start()

    def gather_times(phase, weights):
        totals = [None] * len(weights)
        for piece in range(PIECES + 1):
            if piece < PIECES:
                for d in range(1, n_chip):
                    slot = tp_at(2 * d)
                    hidden_copy(phase, piece, slot, sib).wait_recv()
                    hidden_copy(phase, piece, slot, sib).start()
            if piece == 0:
                continue
            ready = piece - 1
            for d in range(n_chip):
                slot = lax.rem(sib + 2 * d, n_tp)
                hidden_copy(phase, ready, slot, sib).wait_recv()
            whole = hidden[phase, ready]
            if rows % 16:
                whole = whole.astype(F32).reshape(block_rows, span).astype(BF16)
            else:
                whole = whole.reshape(block_rows, span)
            for index, weight in enumerate(weights):
                product = dot(whole, weight[ready * span : (ready + 1) * span, :])
                totals[index] = product if ready == 0 else totals[index] + product
        return totals

    def gather_drain(phase):
        for piece in range(PIECES):
            for _ in range(2 * n_chip - 1):
                hidden_copy(phase, piece, me, sib).wait_send()

    def pair_copy(phase, piece):
        return to_tp(
            part.at[phase, piece, 1 - core], pair_recv.at[phase, piece],
            part_send.at[phase, 0], pair_sem.at[phase, piece], sib,
        )

    def chip_copy(phase, piece, distance, slot):
        other = lax.rem(chip + distance, n_chip)
        return to_tp(
            pair_sum.at[phase, piece, other], part_recv.at[phase, piece, slot],
            part_send.at[phase, 1], part_sem.at[phase, piece, slot], 2 * other + core,
        )

    def scatter_sum(phase, left, weight):
        for piece in range(PIECES):
            product = dot(left, weight[:, piece * span : (piece + 1) * span])
            product = product.reshape(n_chip, 2, rows, span)
            for parity in range(2):
                part[phase, piece, parity] = product[:, parity].astype(BF16)
            pair_copy(phase, piece).start()
        for piece in range(PIECES):
            pair_copy(phase, piece).wait_recv()
            mine = part[phase, piece, core].astype(F32)
            pair_sum[phase, piece] = (mine + pair_recv[phase, piece].astype(F32)).astype(BF16)
            for d in range(1, n_chip):
                chip_copy(phase, piece, d, chip).start()
        sums = []
        for piece in range(PIECES):
            total = pair_sum[phase, piece, chip].astype(F32)
            for d in range(1, n_chip):
                slot = lax.rem(chip + d, n_chip)
                chip_copy(phase, piece, d, slot).wait_recv()
                total = total + part_recv[phase, piece, slot].astype(F32)
            sums.append(total)
        return jnp.concatenate(sums, axis=1)

    def sum_drain(phase):
        for piece in range(PIECES):
            pair_copy(phase, piece).wait_send()
            for d in range(1, n_chip):
                chip_copy(phase, piece, d, chip).wait_send()

    def head_columns(queries):
        blocks = [
            queries[:, h : h + HEAD].T for h in range(0, queries.shape[1], HEAD)
        ]
        return jnp.concatenate(blocks, axis=1).astype(BF16)

    def head_rows(columns):
        blocks = [
            columns[:, c : c + block_rows].T for c in range(0, columns.shape[1], block_rows)
        ]
        return jnp.concatenate(blocks, axis=1).astype(BF16)

    loads[0].wait()
    gather_start(0, normed(target_v[...], pre_first[...]))

    def src_copy(slot, c, device, kind):
        return to_tp(
            src.at[slot, c], src.at[slot, c], src_send.at[kind], src_recv.at[slot, c], device
        )

    loads[1].wait()
    for c in range(CHUNKS):
        src[me, c] = normed(source_v[pl.ds(c * chunk, chunk)], source_gain[...]).astype(BF16)
        for d in range(1, n_chip):
            src_copy(me, c, tp_at(2 * d), 0).start()
        src_copy(me, c, sib, 0).start()

    loads[2].wait()
    q_slots[z] = head_columns(gather_times(0, [query_first])[0])

    def q_copy(distance, slot):
        return to_sp(
            q_slots.at[z], q_slots.at[z] if slot is None else q_slots.at[slot],
            q_sem.at[0, 0], q_sem.at[1, z if slot is None else slot], sp_at(distance),
        )

    for d in range(1, n_sp):
        q_copy(d, None).start()

    loads[3].wait()
    loads[4].wait()

    def project(lines, block, offset):
        first = dot(lines, keyval_first[...])
        second = dot(lines, keyval_second[...])
        place = pl.ds(offset, lines.shape[0])
        k_first[block, place] = first[:, :HEAD].astype(BF16)
        v_first[block, place] = first[:, HEAD:].astype(BF16)
        k_second[z, block, place] = second[:, :HEAD].astype(BF16)
        v_second[z, block, place] = second[:, HEAD:].astype(BF16)

    def project_pair(block, c, mine, other):
        lines = jnp.concatenate([src[mine, c], src[other, c]], axis=0)
        project(lines, block, c * 2 * chunk)

    def absorb(keys, values, queries, slot, fresh):
        scores = dot(keys, queries)
        newest = jnp.max(scores, axis=0, keepdims=True)
        if not fresh:
            newest = jnp.maximum(newest, run_max[slot])
        weights = jnp.exp2((scores - newest) * EXP_SCALE)
        added = jnp.sum(weights, axis=0, keepdims=True)
        gathered = lax.dot_general(
            values, weights.astype(BF16), (((0,), (0,)), ((), ())), preferred_element_type=F32
        )
        if not fresh:
            rescale = jnp.exp2((run_max[slot] - newest) * EXP_SCALE)
            added = added + run_sum[slot] * rescale
            gathered = gathered + run_out[slot] * rescale
        run_max[slot] = newest
        run_sum[slot] = added
        run_out[slot] = gathered

    def absorb_block(block, fresh):
        @pl.loop(0, n_sp)
        def _(slot):
            absorb(k_first[block], v_first[block], q_slots[slot], slot, fresh)

    def kv_copies(block, slot, peer):
        return [
            to_sp(
                store.at[slot, block], store.at[slot, block],
                kv_send.at[index], kv_recv.at[index, slot, block], peer,
            )
            for index, store in enumerate((k_second, v_second))
        ]

    def kv_hop(block, hop, arrive=True, leave=True):
        for step in (1, -1):
            slot = z - step * (hop - 1)
            peer = z + step

            @pl.when(jnp.logical_and(slot >= 0, slot < n_sp))
            def _():
                if arrive:
                    for copy in kv_copies(block, slot, sp_at(1)):
                        copy.wait_recv()
                if leave:

                    @pl.when(jnp.logical_and(hop < n_sp, jnp.logical_and(peer >= 0, peer < n_sp)))
                    def _():
                        for copy in kv_copies(block, slot, peer):
                            copy.start()

    def kv_drain(block, hop):
        for step in (1, -1):
            slot = z - step * (hop - 1)
            peer = z + step
            inside = jnp.logical_and(slot >= 0, slot < n_sp)

            @pl.when(jnp.logical_and(inside, jnp.logical_and(peer >= 0, peer < n_sp)))
            def _():
                for copy in kv_copies(block, slot, peer):
                    copy.wait_send()

    for c in range(CHUNKS):
        src_copy(sib, c, sib, 0).wait_recv()
        project_pair(0, c, me, sib)
    for d in range(1, n_sp):
        q_copy(d, sp_at(d)).wait_recv()
    kv_hop(0, 1, arrive=False)
    absorb_block(0, True)

    def far_chip(d):
        near = tp_at(2 * d)
        far = lax.rem(sib + 2 * d, n_tp)
        for c in range(CHUNKS):
            src_copy(near, c, sib, 1).wait_recv()
            src_copy(near, c, sib, 1).start()
            src_copy(far, c, sib, 1).wait_recv()
            project_pair(d, c, near, far)

    def far_absorb(d):
        far_chip(d)
        absorb_block(d, False)

    times(1, n_chip - 1, far_absorb)
    last = n_chip - 1
    far_chip(last)

    def mix_copies(distance, slot):
        peer = sp_at(distance)
        return [
            to_sp(sent.at[peer], got.at[slot], mix_sem.at[index, 0, 0], mix_sem.at[index, 1, slot], peer)
            for index, (sent, got) in enumerate(((mix_send, mix_recv), (stat_send, stat_recv)))
        ]

    def finish_slot(slot, mixes, stats):
        absorb(k_first[last], v_first[last], q_slots[slot], slot, False)
        total = run_sum[slot]
        mixes[slot] = (run_out[slot] / total).astype(BF16)
        stats[slot] = jnp.concatenate([run_max[slot], total], axis=0)

    @pl.loop(1, n_sp)
    def _(d):
        finish_slot(sp_at(d), mix_send, stat_send)
        for copy in mix_copies(d, z):
            copy.start()

    finish_slot(z, mix_recv, stat_recv)
    for d in range(1, n_sp):
        for copy in mix_copies(d, sp_at(d)):
            copy.wait_recv()
    kv_hop(0, 2)
    for block in range(1, n_chip):
        kv_hop(block, 1, arrive=False)
    top = stat_recv[0, 0:1]
    for slot in range(1, n_sp):
        top = jnp.maximum(top, stat_recv[slot, 0:1])
    weight_sum = jnp.zeros_like(top)
    weighted = jnp.zeros(run_out.shape[1:], F32)
    for slot in range(n_sp):
        share = jnp.exp2((stat_recv[slot, 0:1] - top) * EXP_SCALE) * stat_recv[slot, 1:2]
        weight_sum = weight_sum + share
        weighted = weighted + mix_recv[slot].astype(F32) * share
    loads[5].wait()
    mixed = scatter_sum(0, head_rows(weighted / weight_sum), out_first)
    after_first = target_v[...].astype(F32) + normed(mixed, post_first[...])
    stream[...] = after_first

    gather_start(1, normed(after_first, ffn_pre[...]))
    kv_hop(0, 3)
    for block in range(1, n_chip):
        kv_hop(block, 2)
    loads[6].wait()
    loads[7].wait()
    up_gate, up_value = (up.astype(BF16) for up in gather_times(1, [w_gate, w_value]))
    halo_send[0] = up_gate[block_rows - 16 :]
    halo_send[1] = up_value[block_rows - 16 :]
    halo = to_sp(halo_send, halo_recv, halo_sem.at[0], halo_sem.at[1], sp_at(1))

    @pl.when(z < n_sp - 1)
    def _():
        halo.start()

    @pl.when(z > 0)
    def _():
        halo.wait_recv()

    def causal_mix(up_rows, rim, taps):
        here = up_rows.astype(F32)
        rim = jnp.where(z > 0, rim.astype(F32), 0.0)
        row = lax.broadcasted_iota(jnp.int32, here.shape, 0)
        before = jnp.where(row == 0, rim[15:16], pltpu.roll(here, 1, 0))
        earlier = jnp.where(
            row == 0, rim[14:15], jnp.where(row == 1, rim[15:16], pltpu.roll(here, 2, 0))
        )
        return taps[0:1] * earlier + taps[1:2] * before + taps[2:3] * here

    gated = (
        jax.nn.gelu(causal_mix(up_gate, halo_recv[0], conv_gate[...]), approximate=True)
        * causal_mix(up_value, halo_recv[1], conv_value[...])
    ).astype(BF16)
    loads[8].wait()
    ffn_sum = scatter_sum(1, gated, w_down)
    after_ffn = stream[...] + normed(ffn_sum, ffn_post[...])
    stream[...] = after_ffn

    gather_start(2, normed(after_ffn, pre_second[...]))
    for block in range(1, n_chip):
        kv_hop(block, 3)
    loads[9].wait()
    queries = head_columns(gather_times(2, [query_second])[0])
    for d in range(1, n_sp):
        q_copy(d, None).wait_send()
    q_slots[z] = queries

    for block in range(n_chip):
        absorb(k_second[z, block], v_second[z, block], q_slots[z], 0, block == 0)

    @pl.loop(4, max(n_sp, 4) + 1)
    def _(hop):
        for block in range(n_chip):
            kv_hop(block, hop)

    @pl.loop(1, n_sp)
    def _(d):
        slot = sp_at(d)
        for block in range(n_chip):
            absorb(k_second[slot, block], v_second[slot, block], q_slots[z], 0, False)

    loads[10].wait()
    mixed = scatter_sum(2, head_rows(run_out[0] / run_sum[0]), out_second)
    decoded[...] = stream[...] + normed(mixed, post_second[...])

    for phase in range(3):
        gather_drain(phase)
        sum_drain(phase)
    for c in range(CHUNKS):
        for _ in range(n_chip):
            src_copy(me, c, sib, 0).wait_send()
        for d in range(1, n_chip):
            src_copy(me, c, sib, 1).wait_send()

    def drain(d):
        for block in range(n_chip):
            kv_drain(block, d)
        for copy in mix_copies(d, z):
            copy.wait_send()

    times(1, n_sp, drain)

    @pl.when(z < n_sp - 1)
    def _():
        halo.wait_send()


def per_device(*arrays):
    (target, source, source_gain, pre_first, query_first, keyval_first, out_first, post_first,
     ffn_pre, w_gate, w_value, conv_gate, conv_value, w_down, ffn_post, pre_second,
     query_second, keyval_second, out_second, post_second) = arrays
    n_tp, n_sp = lax.axis_size("tp"), lax.axis_size("sp")
    sharers = 2 * HEAD // keyval_first.shape[1]
    if sharers > 1:
        groups = [list(range(low, low + sharers)) for low in range(0, n_tp, sharers)]
        keyval_first, keyval_second = (
            lax.all_gather(w, "tp", axis=1, tiled=True, axis_index_groups=groups)
            for w in (keyval_first, keyval_second)
        )
    rows, width = target.shape
    lines = source.shape[0]
    block_rows = rows * n_tp
    columns = query_first.shape[1] // HEAD * block_rows
    hidden_units = w_gate.shape[1]
    n_chip = n_tp // 2
    span = width // PIECES
    dma = pltpu.SemaphoreType.DMA
    any_spec = pl.BlockSpec(memory_space=pl.ANY)
    vmem = pl.BlockSpec(memory_space=pltpu.VMEM)

    def row(gain):
        return gain.reshape(1, width)

    scratch = [
        pltpu.VMEM(target.shape, BF16),
        pltpu.VMEM(source.shape, BF16),
        *(pltpu.VMEM(w.shape, BF16) for w in (
            query_first, keyval_first, out_first, w_gate, w_value, w_down,
            query_second, keyval_second, out_second)),
        dma((11,)),
        pltpu.VMEM((3, PIECES, n_tp, rows, span), BF16),
        dma((3,)),
        dma((3, PIECES, n_tp)),
        pltpu.VMEM((n_tp, CHUNKS, lines // CHUNKS, width), BF16),
        dma((2,)),
        dma((n_tp, CHUNKS)),
        pltpu.VMEM((n_sp, HEAD, columns), BF16),
        dma((2, n_sp)),
        pltpu.VMEM((n_chip, 2 * lines, HEAD), BF16),
        pltpu.VMEM((n_chip, 2 * lines, HEAD), BF16),
        pltpu.VMEM((n_sp, n_chip, 2 * lines, HEAD), BF16),
        pltpu.VMEM((n_sp, n_chip, 2 * lines, HEAD), BF16),
        dma((2,)),
        dma((2, n_sp, n_chip)),
        pltpu.VMEM((n_sp, 1, columns), F32),
        pltpu.VMEM((n_sp, 1, columns), F32),
        pltpu.VMEM((n_sp, HEAD, columns), F32),
        pltpu.VMEM((n_sp, HEAD, columns), BF16),
        pltpu.VMEM((n_sp, HEAD, columns), BF16),
        pltpu.VMEM((n_sp, 2, columns), F32),
        pltpu.VMEM((n_sp, 2, columns), F32),
        dma((2, 2, n_sp)),
        pltpu.VMEM((3, PIECES, 2, n_chip, rows, span), BF16),
        pltpu.VMEM((3, PIECES, n_chip, rows, span), BF16),
        pltpu.VMEM((3, PIECES, n_chip, rows, span), BF16),
        pltpu.VMEM((3, PIECES, n_chip, rows, span), BF16),
        dma((3, 2)),
        dma((3, PIECES)),
        dma((3, PIECES, n_chip)),
        pltpu.VMEM((2, 16, hidden_units), BF16),
        pltpu.VMEM((2, 16, hidden_units), BF16),
        dma((2,)),
        pltpu.VMEM((rows, width), F32),
    ]

    def kernel(*refs):
        decoder_kernel(n_tp, n_sp, *refs)

    return pl.pallas_call(
        kernel,
        out_shape=jax.ShapeDtypeStruct((rows, width), F32),
        in_specs=[any_spec, any_spec, vmem, vmem, any_spec, any_spec, any_spec, vmem, vmem,
                  any_spec, any_spec, vmem, vmem, any_spec, vmem, vmem, any_spec, any_spec,
                  any_spec, vmem],
        out_specs=vmem,
        scratch_shapes=scratch,
        compiler_params=pltpu.CompilerParams(
            collective_id=0, has_side_effects=True, vmem_limit_bytes=67_000_000
        ),
        name="decoder",
    )(
        target, source, row(source_gain), row(pre_first), query_first, keyval_first, out_first,
        row(post_first), row(ffn_pre), w_gate, w_value, conv_gate, conv_value, w_down,
        row(ffn_post), row(pre_second), query_second, keyval_second, out_second, row(post_second),
    )


def solution(mesh):
    rows = P(("grp", "sp", "tp"), None)
    by_column, by_row = P(None, "tp"), P("tp", None)
    placed = (
        rows, rows, P(), P(), by_column, by_column, by_row, P(), P(), by_column, by_column,
        by_column, by_column, by_row, P(), P(), by_column, by_column, by_row, P(),
    )
    return jax.shard_map(
        per_device, mesh=mesh, in_specs=placed, out_specs=rows, check_vma=False
    )
```
